32 devices in a mesh: grp: 2 (over y), sp: 4 (over z), tp: 4 (over x, core).
Axes of the slice: x: 2, y: 2, z: 4, core: 2. Of those that a mesh axis runs over, the one named last changes fastest.
Arguments:
- tokens: bfloat16 [4096, 2048], P(('grp', 'sp', 'tp')), parts along dimension 0, may hold values from -6 to 6
- norm_gain: bfloat16 [2048], replicated, may hold values from 0.099609375 to 1.8984375
- conv_outer_weight: bfloat16 [2048, 1024], P('sp', 'tp'), may hold values from -0.125 to 0.125
- conv_inner_weight: bfloat16 [2048, 1024], P('sp', 'tp'), may hold values from -0.125 to 0.125
- conv_input_weight: bfloat16 [2048, 1024], P('sp', 'tp'), may hold values from -0.125 to 0.125
- query_matrix: bfloat16 [2048, 1024], P('sp', 'tp'), may hold values from -0.125 to 0.125
- key_weight: bfloat16 [2048, 1024], P('sp', 'tp'), may hold values from -0.125 to 0.125
- value_weight: bfloat16 [2048, 1024], P('sp', 'tp'), may hold values from -0.125 to 0.125
- gate_weight: bfloat16 [2048, 1024], P('sp', 'tp'), may hold values from -0.125 to 0.125
- conv_taps: bfloat16 [3, 1024], P(None, 'tp'), may hold values from -3.5 to 3.5
- conv_out_weight: bfloat16 [1024, 2048], P('tp', 'sp'), may hold values from -0.125 to 0.125
- ret_out_weight: bfloat16 [1024, 2048], P('tp', 'sp'), may hold values from -0.125 to 0.125
- log_decay: float32 [4096, 8], P(('grp', 'sp'), 'tp'), parts along dimension 0, may hold values from -0.75 to 0
Outputs:
- mixed: bfloat16 [4096, 2048], P(('grp', 'sp', 'tp')), parts along dimension 0
The draws below stay inside these ranges and needn't reach their ends.
There are 2 independent parts, one for each index of `grp`. The reference program is written for one: setup_inputs(seed, part) draws one part's arguments, and reference() takes and returns one part's arrays. A program takes and returns all parts, laid end to end along the dimension named above; an argument that names none is the same for every part. Nothing has to cross between parts.
All inputs are finite; a program needn't handle non-finite values.
Results may differ from the reference program's by a relative error of at most 0.025.
Values may be sent and summed in bfloat16 or wider, within the bound.
A program may use at most 64 MiB of HBM per device.

```python
import math
import jax
import jax.numpy as jnp
from jax import lax

D = 2048
CONV_W = 1024
RET_HEADS = 8
HEAD = 128
CONV_K = 3
BLOCK = 128
TOK_SP = 512
RET_W = 1024
SEQUENCE_TOKENS = 2048
N_TP = 4


def draw_log_decay(key, part):
    folded = jax.random.fold_in(key, 17)
    random_subkeys = jax.random.split(folded, 7)
    ranking = jax.random.permutation(random_subkeys[0], RET_HEADS)
    fast_count = RET_HEADS // 2
    is_fast = (ranking < fast_count).astype(jnp.float32)
    fast_rate = jnp.exp(jax.random.uniform(random_subkeys[1], (RET_HEADS,), jnp.float32, math.log(1.0 / 100.0), math.log(1.0 / 30.0)))
    slow_rate = jnp.exp(jax.random.uniform(random_subkeys[2], (RET_HEADS,), jnp.float32, math.log(0.02), math.log(0.3))) / SEQUENCE_TOKENS
    rates = is_fast * fast_rate + (1.0 - is_fast) * slow_rate
    span_count = SEQUENCE_TOKENS // TOK_SP
    span_factor = jnp.exp(jax.random.uniform(random_subkeys[3], (span_count,), jnp.float32, math.log(0.5), math.log(2.0)))
    span_index = jnp.arange(SEQUENCE_TOKENS, dtype=jnp.int32) // TOK_SP
    position_factor = span_factor[span_index]
    jitter = jax.random.uniform(random_subkeys[4], (SEQUENCE_TOKENS, RET_HEADS), jnp.float32, 0.5, 1.5)
    decay_values = -rates[None, :] * position_factor[:, None] * jitter
    spike_position = jax.random.permutation(random_subkeys[5], SEQUENCE_TOKENS)[:3].astype(jnp.int32)
    spike_log_decay = jnp.log(jax.random.uniform(random_subkeys[6], (3,), jnp.float32, 0.55, 0.8))
    spike_reached = (jnp.arange(SEQUENCE_TOKENS, dtype=jnp.int32)[:, None] == spike_position[None, :]).astype(jnp.float32)
    decay_values = decay_values + jnp.sum(spike_reached * spike_log_decay[None, :], axis=1)[:, None]
    return decay_values.astype(jnp.float32)


def level_of(key, dims, shards, smallest, high):
    gain, own = 1.0, jax.random.fold_in(key, 6)
    for axis_at, parts in shards:
        heights = jnp.exp(jax.random.uniform(jax.random.fold_in(own, axis_at), (parts,), jnp.float32, smallest / len(shards), high / len(shards)))
        gain = gain * jnp.repeat(heights, dims[axis_at] // parts).reshape([-1 if axis == axis_at else 1 for axis in range(len(dims))])
    return gain


def normal_values(key, dims, scale, limit, cuts=(), kind=jnp.bfloat16):
    entries = jax.random.normal(key, dims, jnp.float32) * scale
    if len(cuts) > 0:
        entries = level_of(key, dims, cuts, -0.22, 0.18) * entries
    return jnp.clip(entries, min=-limit, max=limit).astype(kind)


def setup_inputs(seed: int = 0, part: int = 0) -> dict:
    seeds = jax.random.split(jax.random.key(seed), 14)
    part_keys = jax.random.split(jax.random.fold_in(seeds[13], part), 14)
    tokens = normal_values(part_keys[0], (SEQUENCE_TOKENS, D), 1.0, 6.0, ((0, 16),))
    norm_gain = jnp.clip(1.0 + 0.18 * jax.random.normal(seeds[1], (D,), jnp.float32), 0.099609375, 1.8984375).astype(jnp.bfloat16)
    conv_outer_weight = normal_values(seeds[2], (D, CONV_W), D ** -0.5, 0.125, ((0, 4), (1, 4)))
    conv_inner_weight = normal_values(seeds[3], (D, CONV_W), D ** -0.5, 0.125, ((0, 4), (1, 4)))
    conv_input_weight = normal_values(seeds[4], (D, CONV_W), D ** -0.5, 0.125, ((0, 4), (1, 4)))
    query_matrix = normal_values(seeds[5], (D, RET_W), D ** -0.5, 0.125, ((0, 4), (1, 4)))
    key_weight = normal_values(seeds[6], (D, RET_W), D ** -0.5, 0.125, ((0, 4), (1, 4)))
    value_weight = normal_values(seeds[7], (D, RET_W), D ** -0.5, 0.125, ((0, 4), (1, 4)))
    gate_weight = normal_values(seeds[8], (D, RET_W), D ** -0.5, 0.125, ((0, 4), (1, 4)))
    conv_taps = normal_values(seeds[9], (CONV_K, CONV_W), CONV_K ** -0.5, 3.5, ((1, 4),))
    conv_out_weight = normal_values(seeds[10], (CONV_W, D), (CONV_W + RET_W) ** -0.5, 0.125, ((0, 4), (1, 4)))
    ret_out_weight = normal_values(seeds[11], (RET_W, D), (CONV_W + RET_W) ** -0.5, 0.125, ((0, 4), (1, 4)))
    log_decay = draw_log_decay(jax.random.fold_in(jax.random.fold_in(seeds[13], part), 71), part)
    return {"tokens": tokens, "norm_gain": norm_gain, "conv_outer_weight": conv_outer_weight, "conv_inner_weight": conv_inner_weight, "conv_input_weight": conv_input_weight, "query_matrix": query_matrix, "key_weight": key_weight, "value_weight": value_weight, "gate_weight": gate_weight, "conv_taps": conv_taps, "conv_out_weight": conv_out_weight, "ret_out_weight": ret_out_weight, "log_decay": log_decay}


EPSILON = 1e-06
ROTARY_BASE = 10000.0
HIGHEST_PRECISION = lax.Precision.HIGHEST

def rotate(head_data, positions):
    half_width = head_data.shape[-1] // 2
    inv_freq = ROTARY_BASE ** (-jnp.arange(half_width, dtype=jnp.float32) / half_width)
    angles = positions[:, None] * inv_freq[None, :]
    cosine = jnp.cos(angles)[:, None, :]
    sine_part = jnp.sin(angles)[:, None, :]
    first_half = head_data[..., :half_width]
    second_half = head_data[..., half_width:]
    return jnp.concatenate([first_half * cosine - second_half * sine_part, second_half * cosine + first_half * sine_part], axis=-1)

def head_norm(head_data):
    return head_data * lax.rsqrt(lax.optimization_barrier(jnp.mean(head_data * head_data, axis=-1, keepdims=True)) + EPSILON)

def retain(queries, keys_rot, head_values, log_decay):
    block_count = SEQUENCE_TOKENS // BLOCK
    block_shape = (block_count, BLOCK, RET_HEADS, HEAD)
    offsets = jnp.arange(BLOCK, dtype=jnp.int32)
    causal_mask = (offsets[:, None] >= offsets[None, :])[:, :, None]

    def block_step(carried, pieces):
        query_block, key_block, value_block, log_block = pieces
        cumulative = jnp.cumsum(log_block, axis=0)
        spread = cumulative[:, None, :] - cumulative[None, :, :]
        decay_grid = jnp.where(causal_mask, jnp.exp(jnp.where(causal_mask, spread, 0.0)), 0.0)
        scores = jnp.einsum('ihd,jhd->ijh', query_block, key_block, precision=HIGHEST_PRECISION) * decay_grid
        within = jnp.einsum('ijh,jhe->ihe', scores, value_block, precision=HIGHEST_PRECISION)
        across = jnp.einsum('ihd,hde->ihe', query_block, carried, precision=HIGHEST_PRECISION)
        across = across * jnp.exp(cumulative)[:, :, None]
        block_end = cumulative[-1]
        weights = jnp.exp(block_end[None, :] - cumulative)
        increment = jnp.einsum('jh,jhd,jhe->hde', weights, key_block, value_block, precision=HIGHEST_PRECISION)
        updated = jnp.exp(block_end)[:, None, None] * carried + increment
        return (updated, within + across)
    start_state = jnp.zeros((RET_HEADS, HEAD, HEAD), jnp.float32)
    _, outputs = lax.scan(block_step, start_state, (queries.reshape(block_shape), keys_rot.reshape(block_shape), head_values.reshape(block_shape), log_decay.reshape(block_count, BLOCK, RET_HEADS)))
    return outputs.reshape(SEQUENCE_TOKENS, RET_HEADS, HEAD)

def reference(tokens, norm_gain, conv_outer_weight, conv_inner_weight, conv_input_weight, query_matrix, key_weight, value_weight, gate_weight, conv_taps, conv_out_weight, ret_out_weight, log_decay):
    values32 = tokens.astype(jnp.float32)
    normed = (values32 * lax.rsqrt(lax.optimization_barrier(jnp.mean(values32 * values32, axis=-1, keepdims=True)) + EPSILON) * norm_gain.astype(jnp.float32)).astype(jnp.bfloat16)

    def project(weight):
        return jnp.dot(normed, weight, preferred_element_type=jnp.float32).astype(jnp.bfloat16)
    conv_outer = project(conv_outer_weight)
    conv_inner = project(conv_inner_weight)
    conv_input = project(conv_input_weight)
    query_proj = project(query_matrix)
    key_proj = project(key_weight)
    value_proj = project(value_weight)
    gate_proj = project(gate_weight)
    mixed_in = conv_inner.astype(jnp.float32) * conv_input.astype(jnp.float32)
    extended = jnp.concatenate([jnp.zeros((CONV_K - 1, CONV_W), jnp.float32), mixed_in], axis=0)
    taps = conv_taps.astype(jnp.float32)
    conv_out = jnp.zeros((SEQUENCE_TOKENS, CONV_W), jnp.float32)
    for tap_index in range(CONV_K):
        conv_out = conv_out + taps[tap_index][None, :] * extended[tap_index:tap_index + SEQUENCE_TOKENS]
    conv_branch = (conv_outer.astype(jnp.float32) * conv_out).astype(jnp.bfloat16)
    positions = jnp.arange(SEQUENCE_TOKENS, dtype=jnp.float32)
    head_shape = (SEQUENCE_TOKENS, RET_HEADS, HEAD)
    queries = rotate(query_proj.astype(jnp.float32).reshape(head_shape), positions)
    keys_rot = rotate(key_proj.astype(jnp.float32).reshape(head_shape), positions) * HEAD ** (-0.5)
    head_values = value_proj.astype(jnp.float32).reshape(head_shape)
    retained = retain(queries, keys_rot, head_values, log_decay)
    ret_branch = (head_norm(retained).reshape(SEQUENCE_TOKENS, RET_W) * jax.nn.silu(gate_proj.astype(jnp.float32))).astype(jnp.bfloat16)
    conv_group = CONV_W // N_TP
    ret_group = RET_W // N_TP
    summed = jnp.zeros((SEQUENCE_TOKENS, D), jnp.float32)
    for group_index in range(N_TP):
        conv_lo = group_index * conv_group
        ret_lo = group_index * ret_group
        partial_term = jnp.dot(conv_branch[:, conv_lo:conv_lo + conv_group], conv_out_weight[conv_lo:conv_lo + conv_group], preferred_element_type=jnp.float32)
        partial_term = partial_term + jnp.dot(ret_branch[:, ret_lo:ret_lo + ret_group], ret_out_weight[ret_lo:ret_lo + ret_group], preferred_element_type=jnp.float32)
        summed = summed + partial_term.astype(jnp.bfloat16).astype(jnp.float32)
    return summed.astype(jnp.bfloat16)
```

```python
import functools

import jax
import jax.numpy as jnp
from jax import lax
from jax.experimental import pallas as pl
from jax.experimental.pallas import tpu as pltpu
from jax.sharding import PartitionSpec as P

HEAD = 128
CONV_K = 3
BLOCK = 128


EPSILON = 1e-06
ROTARY_BASE = 10000.0
HIGHEST_PRECISION = lax.Precision.HIGHEST


def prefix_2(x, axis, join, neutral):
    place = lax.axis_index(axis)
    gathered = jax.tree.map(
        lambda a, kind: lax.all_gather(a.astype(kind), axis), x, (jnp.bfloat16, jnp.bfloat16)
    )
    state = jax.tree.map(lambda a, e: jnp.zeros_like(a) + jnp.asarray(e, a.dtype), x, neutral)

    def one(turn, state):
        return join(
            state,
            jax.tree.map(
                lambda a, own: lax.dynamic_index_in_dim(a, turn, 0, False).astype(own.dtype),
                gathered,
                x,
            ),
        )

    return lax.fori_loop(0, place, one, state)


def shifted(x, axis, by):
    count = lax.axis_size(axis)
    pairs = [(i, i + by) for i in range(count) if 0 <= i + by < count]
    return lax.ppermute(x, axis, pairs)


def rotate(head_data, positions):
    half_width = head_data.shape[-1] // 2
    inv_freq = ROTARY_BASE ** (-jnp.arange(half_width, dtype=jnp.float32) / half_width)
    angles = positions[:, None] * inv_freq[None, :]
    cosine = jnp.cos(angles)[:, None, :]
    sine_part = jnp.sin(angles)[:, None, :]
    first_half = head_data[..., :half_width]
    second_half = head_data[..., half_width:]
    return jnp.concatenate(
        [
            first_half * cosine - second_half * sine_part,
            second_half * cosine + first_half * sine_part,
        ],
        axis=-1,
    )


def head_norm(head_data):
    return head_data * lax.rsqrt(jnp.mean(head_data * head_data, axis=-1, keepdims=True) + EPSILON)


def combine_states(earlier, later):
    return (earlier[0] * later[0], later[0][:, None, None] * earlier[1] + later[1])


def body(
    tokens,
    norm_gain,
    conv_outer_weight,
    conv_inner_weight,
    conv_input_weight,
    query_matrix,
    key_weight,
    value_weight,
    gate_weight,
    conv_taps,
    conv_out_weight,
    ret_out_weight,
    log_decay,
):
    values32 = tokens.astype(jnp.float32)
    normed = (
        values32
        * lax.rsqrt(jnp.mean(values32 * values32, axis=-1, keepdims=True) + EPSILON)
        * norm_gain.astype(jnp.float32)
    ).astype(jnp.bfloat16)
    gathered = lax.all_gather(normed, "tp", axis=0, tiled=True)
    row_total = gathered.shape[0]
    whole = (
        lax.all_gather(conv_outer_weight, "sp", axis=0, tiled=True),
        lax.all_gather(conv_inner_weight, "sp", axis=0, tiled=True),
        lax.all_gather(conv_input_weight, "sp", axis=0, tiled=True),
        lax.all_gather(query_matrix, "sp", axis=0, tiled=True),
        lax.all_gather(key_weight, "sp", axis=0, tiled=True),
        lax.all_gather(value_weight, "sp", axis=0, tiled=True),
        lax.all_gather(gate_weight, "sp", axis=0, tiled=True),
    )
    projected = tuple(
        (
            jnp.dot(gathered, weight, preferred_element_type=jnp.float32).astype(jnp.bfloat16)
            for weight in whole
        )
    )
    conv_outer, conv_inner, conv_input, query_proj, key_proj, value_proj, gate_proj = projected
    heads_here = query_proj.shape[1] // HEAD
    offset = (lax.axis_index("sp") * row_total).astype(jnp.float32)
    positions = offset + jnp.arange(row_total, dtype=jnp.float32)
    head_shape = (row_total, heads_here, HEAD)
    queries = rotate(query_proj.astype(jnp.float32).reshape(head_shape), positions)
    keys_rot = rotate(key_proj.astype(jnp.float32).reshape(head_shape), positions) * HEAD ** (-0.5)
    head_values = value_proj.astype(jnp.float32).reshape(head_shape)
    block_count = row_total // BLOCK
    block_shape = (block_count, BLOCK, heads_here, HEAD)
    query_blocks = queries.reshape(block_shape)
    key_blocks = keys_rot.reshape(block_shape)
    value_blocks = head_values.reshape(block_shape)
    log_blocks = log_decay.reshape(block_count, BLOCK, heads_here)
    offsets = jnp.arange(BLOCK, dtype=jnp.int32)
    causal_mask = offsets[:, None] >= offsets[None, :]
    lower_ones = causal_mask.astype(jnp.float32)
    cumulative = jnp.einsum("ij,njh->nih", lower_ones, log_blocks, precision=HIGHEST_PRECISION)
    block_end = cumulative[:, -1, :]
    mixed_in = conv_inner.astype(jnp.float32) * conv_input.astype(jnp.float32)
    rim = shifted(mixed_in[row_total - (CONV_K - 1) :], "sp", 1)
    extended = jnp.concatenate([rim, mixed_in], axis=0)
    taps = conv_taps.astype(jnp.float32)
    conv_out = jnp.zeros(mixed_in.shape, jnp.float32)
    for tap_index in range(CONV_K):
        conv_out = conv_out + taps[tap_index][None, :] * extended[tap_index : tap_index + row_total]
    conv_branch = (conv_outer.astype(jnp.float32) * conv_out).astype(jnp.bfloat16)
    weights = jnp.exp(block_end[:, None, :] - cumulative)
    increments = jnp.einsum(
        "njh,njhd,njhe->nhde", weights, key_blocks, value_blocks, precision=HIGHEST_PRECISION
    )

    def carry_on(carried, pieces):
        block_decay, increment = pieces
        return (block_decay[:, None, None] * carried + increment, carried)

    start_state = jnp.zeros((heads_here, HEAD, HEAD), jnp.float32)
    local_end, local_before = lax.scan(carry_on, start_state, (jnp.exp(block_end), increments))
    device_decay = jnp.exp(jnp.sum(block_end, axis=0))
    incoming = prefix_2(
        (device_decay, local_end),
        "sp",
        combine_states,
        (jnp.ones_like(device_decay), jnp.zeros_like(local_end)),
    )
    local_before, incoming_state = (local_before, incoming[1])
    spread = cumulative[:, :, None, :] - cumulative[:, None, :, :]
    grid_mask = causal_mask[None, :, :, None]
    decay_grid = jnp.where(grid_mask, jnp.exp(jnp.where(grid_mask, spread, 0.0)), 0.0)
    scores = (
        jnp.einsum("nihd,njhd->nijh", query_blocks, key_blocks, precision=HIGHEST_PRECISION)
        * decay_grid
    )
    within = jnp.einsum("nijh,njhe->nihe", scores, value_blocks, precision=HIGHEST_PRECISION)
    prefix = jnp.exp(jnp.cumsum(block_end, axis=0) - block_end)
    before = local_before + prefix[:, :, None, None] * incoming_state[None]
    across = jnp.einsum("nihd,nhde->nihe", query_blocks, before, precision=HIGHEST_PRECISION)
    across = across * jnp.exp(cumulative)[..., None]
    retained = (within + across).reshape(head_shape)
    ret_branch = (
        head_norm(retained).reshape(row_total, heads_here * HEAD)
        * jax.nn.silu(gate_proj.astype(jnp.float32))
    ).astype(jnp.bfloat16)
    conv_rows_weight, ret_rows_weight = (
        lax.all_gather(conv_out_weight, "sp", axis=1, tiled=True),
        lax.all_gather(ret_out_weight, "sp", axis=1, tiled=True),
    )
    return lax.psum_scatter(
        (
            jnp.dot(conv_branch, conv_rows_weight, preferred_element_type=jnp.float32)
            + jnp.dot(ret_branch, ret_rows_weight, preferred_element_type=jnp.float32)
        ).astype(jnp.bfloat16),
        "tp",
        scatter_dimension=0,
        tiled=True,
    )


MESH = pl.DeviceIdType.MESH
NPROJ = 7
LAG = 2
ORDER = (3, 4, 5, 6, 0, 1, 2)
QUERY, KEY, VALUE, GATE, OUTER, INNER, INPUT = range(NPROJ)


def remote(src, dst, send, recv, axis, to):
    return pltpu.make_async_remote_copy(
        src_ref=src, dst_ref=dst, send_sem=send, recv_sem=recv, device_id={axis: to}, device_id_type=MESH
    )


def kernel(sizes, *refs):
    n, g, m = sizes
    tokens, gain, w0, w1, w2, w3, w4, w5, w6, taps, oc, orr, ld, ldt, cos2, sin2, out = refs[:17]
    (raw, xn, gw, go, acc, ext, qr, kr, cum_s, cumt_s, lend, dec, instate, indec, sin_s, rb, cb, stage, land, tail, own) = refs[17:38]
    (tsend, trecv, rsend, lsend, zrecv, ysend, yrecv, ssend, srecv, dsend, drecv, csend, crecv, osend, orecv) = refs[38:]
    weights = [(w0, w1, w2, w3, w4, w5, w6)[i] for i in ORDER]
    outs = (oc, orr)
    me = lax.axis_index("sp")
    grp = lax.axis_index("grp")
    mine = lax.axis_index("tp")
    rows, width = tokens.shape
    total = rows * m
    depth, cols = w0.shape
    half = depth // 2
    orows = oc.shape[0]
    ohalf = orows // 2
    ocols = oc.shape[1]
    heads = cols // HEAD
    other = 1 - grp

    barrier = pltpu.get_barrier_semaphore()
    for axis, count, at in (("sp", n, me), ("grp", g, grp), ("tp", m, mine)):
        for d in range(1, count):
            pl.semaphore_signal(barrier, inc=1, device_id={axis: lax.rem(at + d, count)}, device_id_type=MESH)
    pl.semaphore_wait(barrier, n + g + m - 3)

    def token_copy(d):
        to = lax.rem(mine + d, m)
        return remote(tokens, raw.at[d - 1], tsend.at[d - 1], trecv.at[d - 1], "tp", to)

    for d in range(1, m):
        token_copy(d).start()

    hs = pl.ds(pl.multiple_of(grp * half, half), half)
    ohs = pl.ds(pl.multiple_of(grp * ohalf, ohalf), ohalf)

    def slot(w, s, is_out):
        return go.at[w, s, ohs] if is_out else gw.at[w, s, hs]

    def sem_at(w, is_out):
        return w + NPROJ if is_out else w

    def line_copy(w, s, is_out, right, src=None):
        dst = slot(w, s, is_out)
        k = sem_at(w, is_out)
        to = me + 1 if right else me - 1
        return remote(
            dst if src is None else src, dst, (rsend if right else lsend).at[k, s], zrecv.at[k, s], "sp", to
        )

    def pair_copy(w, s, is_out):
        part = slot(w, s, is_out)
        k = sem_at(w, is_out)
        return remote(part, part, ysend.at[k, s], yrecv.at[k, s], "grp", other)

    for w, is_out in [(0, True), (1, True)] + [(w, False) for w in range(NPROJ)]:
        src = outs[w].at[ohs] if is_out else weights[w].at[hs]

        @pl.when(me < n - 1)
        def _():
            line_copy(w, me, is_out, True, src).start()

        @pl.when(me > 0)
        def _():
            line_copy(w, me, is_out, False, src).start()

    below = lax.broadcasted_iota(jnp.int32, (total, total), 0) >= lax.broadcasted_iota(jnp.int32, (total, total), 1)
    cum_s[...] = jnp.dot(below.astype(jnp.float32), ld[...], precision=HIGHEST_PRECISION, preferred_element_type=jnp.float32)
    above = lax.broadcasted_iota(jnp.int32, (total, total), 0) <= lax.broadcasted_iota(jnp.int32, (total, total), 1)
    cumt_s[...] = jnp.dot(ldt[...], above.astype(jnp.float32), precision=HIGHEST_PRECISION, preferred_element_type=jnp.float32)

    step_rows = 16
    scale = gain[...].astype(jnp.float32)

    def normalise(source, block):
        def one(i, carry):
            at = pl.multiple_of(i * step_rows, step_rows)
            v = source[pl.ds(at, step_rows), :].astype(jnp.float32)
            r = lax.rsqrt(jnp.mean(v * v, axis=-1, keepdims=True) + EPSILON)
            y = (v * r * scale).astype(jnp.bfloat16)
            to = pl.ds(pl.multiple_of(block * rows + at, step_rows), step_rows)
            for s in range(n):
                xn[s, to, :] = y[:, s * depth : (s + 1) * depth]
            return carry

        lax.fori_loop(0, rows // step_rows, one, 0)

    normalise(tokens, mine)
    for d in range(1, m):
        token_copy(d).wait_recv()
        normalise(raw.at[d - 1], lax.rem(mine - d + m, m))

    for w in range(NPROJ):
        acc[w] = jnp.dot(xn[me], weights[w][...], preferred_element_type=jnp.float32)
    for w in range(2):
        go[w, me] = outs[w][...]

    def forward(w, is_out, d):
        @pl.when(me >= d)
        def _():
            s = me - d
            line_copy(w, s, is_out, True).wait_recv()

            @pl.when(me < n - 1)
            def _():
                line_copy(w, s, is_out, True).start()

            pair_copy(w, s, is_out).start()

        @pl.when(me + d < n)
        def _():
            s = me + d
            line_copy(w, s, is_out, False).wait_recv()

            @pl.when(me > 0)
            def _():
                line_copy(w, s, is_out, False).start()

            pair_copy(w, s, is_out).start()

    def other_wait(w, s, is_out):
        theirs = (
            go.at[w, s, pl.ds(pl.multiple_of(other * ohalf, ohalf), ohalf)]
            if is_out
            else gw.at[w, s, pl.ds(pl.multiple_of(other * half, half), half)]
        )
        k = sem_at(w, is_out)
        remote(theirs, theirs, ysend.at[k, s], yrecv.at[k, s], "grp", other).wait_recv()

    def consume(w, d):
        @pl.when(me >= d)
        def _():
            s = me - d
            other_wait(w, s, False)
            acc[w] += jnp.dot(xn[s], gw[w, s], preferred_element_type=jnp.float32)

        @pl.when(me + d < n)
        def _():
            s = me + d
            other_wait(w, s, False)
            acc[w] += jnp.dot(xn[s], gw[w, s], preferred_element_type=jnp.float32)

    def phase(d, lo, hi):
        def one(i, carry):
            @pl.when(i < hi)
            def _():
                forward(i, False, d)

            @pl.when(i >= lo + LAG)
            def _():
                consume(i - LAG, d)

            return carry

        lax.fori_loop(lo, hi + LAG, one, 0)

    for d in range(1, n):
        forward(0, True, d)
        forward(1, True, d)
        if d < n - 1:
            phase(d, 0, NPROJ)
    phase(n - 1, 0, 3)

    def projected(w, h=None):
        part = acc[w] if h is None else acc[w, :, h * HEAD : (h + 1) * HEAD]
        return part.astype(jnp.bfloat16).astype(jnp.float32)

    def state_copy(d):
        return remote(lend, instate.at[me], ssend.at[d - 1], srecv.at[me], "sp", me + d)

    def decay_copy(d):
        return remote(dec, indec.at[me], dsend.at[d - 1], drecv.at[me], "sp", me + d)

    dec[...] = jnp.zeros_like(dec)
    for h in range(heads):
        k = projected(KEY, h)
        k = (k * cos2[...] + pltpu.roll(k, HEAD // 2, 1) * sin2[...]) * HEAD ** (-0.5)
        kr[h] = k.astype(jnp.bfloat16)
        q = projected(QUERY, h)
        qr[h] = (q * cos2[...] + pltpu.roll(q, HEAD // 2, 1) * sin2[...]).astype(jnp.bfloat16)
        c = cum_s[:, h : h + 1]
        end = cum_s[total - 1 : total, h : h + 1]
        kw = (k * jnp.exp(end - c)).astype(jnp.bfloat16)
        vals = acc[VALUE, :, h * HEAD : (h + 1) * HEAD].astype(jnp.bfloat16)
        lend[h] = lax.dot_general(kw, vals, (((0,), (0,)), ((), ())), preferred_element_type=jnp.float32).astype(jnp.bfloat16)
        dec[h : h + 1, :] = jnp.broadcast_to(end, (1, HEAD))
    for d in range(1, n):

        @pl.when(me + d < n)
        def _():
            state_copy(d).start()
            decay_copy(d).start()

    phase(n - 1, 3, NPROJ)

    mixed_in = projected(INNER) * projected(INPUT)
    ext[8:, :] = mixed_in
    tail[...] = mixed_in[total - 8 :, :]

    def rim_copy():
        return remote(tail, ext.at[0:8], csend, crecv, "sp", me + 1)

    @pl.when(me < n - 1)
    def _():
        rim_copy().start()

    sin_s[...] = jnp.zeros_like(sin_s)
    for s in range(n - 1):

        @pl.when(me > s)
        def _():
            remote(lend, instate.at[s], ssend.at[0], srecv.at[s], "sp", s).wait_recv()
            remote(dec, indec.at[s], dsend.at[0], drecv.at[s], "sp", s).wait_recv()
            for h in range(heads):
                sin_s[h] = jnp.exp(indec[s, h : h + 1, :]) * sin_s[h] + instate[s, h].astype(jnp.float32)

    for h in range(heads):
        c = cum_s[:, h : h + 1]
        spread = c - cumt_s[h : h + 1, :]
        grid = jnp.where(below, jnp.exp(jnp.where(below, spread, 0.0)), 0.0)
        scores = lax.dot_general(qr[h], kr[h], (((1,), (1,)), ((), ())), preferred_element_type=jnp.float32) * grid
        vals = acc[VALUE, :, h * HEAD : (h + 1) * HEAD].astype(jnp.bfloat16)
        kept = jnp.dot(scores.astype(jnp.bfloat16), vals, preferred_element_type=jnp.float32)
        kept += jnp.dot(qr[h], sin_s[h].astype(jnp.bfloat16), preferred_element_type=jnp.float32) * jnp.exp(c)
        gate = projected(GATE, h)
        normed = kept * lax.rsqrt(jnp.mean(kept * kept, axis=-1, keepdims=True) + EPSILON)
        rb[:, h * HEAD : (h + 1) * HEAD] = (normed * (gate / (1.0 + jnp.exp(-gate)))).astype(jnp.bfloat16)

    @pl.when(me > 0)
    def _():
        remote(tail, ext.at[0:8], csend, crecv, "sp", me - 1).wait_recv()

    @pl.when(me == 0)
    def _():
        ext[0:8, :] = jnp.zeros((8, cols), jnp.float32)

    t = taps[...].astype(jnp.float32)
    conv = jnp.zeros((total, cols), jnp.float32)
    for j in range(CONV_K):
        lo = 8 - (CONV_K - 1) + j
        conv = conv + t[j : j + 1, :] * ext[lo : lo + total, :]
    cb[...] = (projected(OUTER) * conv).astype(jnp.bfloat16)

    for d in range(1, n):
        for w in range(2):

            @pl.when(me >= d)
            def _():
                other_wait(w, me - d, True)

            @pl.when(me + d < n)
            def _():
                other_wait(w, me + d, True)

    def partial(block, s):
        at = pl.ds(pl.multiple_of(block * rows, rows), rows)
        return jnp.dot(cb[at, :], go[0, s], preferred_element_type=jnp.float32) + jnp.dot(
            rb[at, :], go[1, s], preferred_element_type=jnp.float32
        )

    def out_copy(d):
        return remote(stage.at[d - 1], land.at[d - 1], osend.at[d - 1], orecv.at[d - 1], "tp", lax.rem(mine + d, m))

    for d in range(1, m):
        block = lax.rem(mine + d, m)
        for s in range(n):
            stage[d - 1, :, s * ocols : (s + 1) * ocols] = partial(block, s).astype(jnp.bfloat16)
        out_copy(d).start()
    for s in range(n):
        own[:, s * ocols : (s + 1) * ocols] = partial(mine, s)
    for d in range(1, m):
        out_copy(d).wait_recv()
    for s in range(n):
        at = slice(s * ocols, (s + 1) * ocols)
        value = own[:, at].astype(jnp.bfloat16).astype(jnp.float32)
        for d in range(1, m):
            value = value + land[d - 1, :, at].astype(jnp.float32)
        out[:, at] = value.astype(jnp.bfloat16)

    for d in range(1, m):
        token_copy(d).wait_send()
        out_copy(d).wait_send()
    for d in range(1, n):

        @pl.when(me + d < n)
        def _():
            state_copy(d).wait_send()
            decay_copy(d).wait_send()

    @pl.when(me < n - 1)
    def _():
        rim_copy().wait_send()

    for is_out, count in ((True, 2), (False, NPROJ)):

        def drain(w, carry):
            for s in range(n):

                @pl.when((s <= me) & (me < n - 1))
                def _():
                    line_copy(w, s, is_out, True).wait_send()

                @pl.when((s >= me) & (me > 0))
                def _():
                    line_copy(w, s, is_out, False).wait_send()

                @pl.when(me != s)
                def _():
                    pair_copy(w, s, is_out).wait_send()

            return carry

        lax.fori_loop(0, count, drain, 0)


def fused(sizes, *args):
    n, g, m = sizes
    tokens, gain, w0 = args[0], args[1], args[2]
    log_decay = args[12]
    rows, width = tokens.shape
    depth, cols = w0.shape
    orows, ocols = args[10].shape
    total = rows * m
    heads = cols // HEAD
    half_width = HEAD // 2
    inv_freq = ROTARY_BASE ** (-jnp.arange(half_width, dtype=jnp.float32) / half_width)
    offset = (lax.axis_index("sp") * total).astype(jnp.float32)
    angles = (offset + jnp.arange(total, dtype=jnp.float32))[:, None] * inv_freq[None, :]
    cosine, sine = jnp.cos(angles), jnp.sin(angles)
    cos2 = jnp.concatenate([cosine, cosine], axis=1)
    sin2 = jnp.concatenate([-sine, sine], axis=1)
    bf, f32 = jnp.bfloat16, jnp.float32
    dma = pltpu.SemaphoreType.DMA
    scratch = [
        pltpu.VMEM((m - 1, rows, width), bf),
        pltpu.VMEM((n, total, depth), bf),
        pltpu.VMEM((NPROJ, n, depth, cols), bf),
        pltpu.VMEM((2, n, orows, ocols), bf),
        pltpu.VMEM((NPROJ, total, cols), f32),
        pltpu.VMEM((total + 8, cols), f32),
        pltpu.VMEM((heads, total, HEAD), bf),
        pltpu.VMEM((heads, total, HEAD), bf),
        pltpu.VMEM((total, heads), f32),
        pltpu.VMEM((heads, total), f32),
        pltpu.VMEM((heads, HEAD, HEAD), bf),
        pltpu.VMEM((8, HEAD), f32),
        pltpu.VMEM((n, heads, HEAD, HEAD), bf),
        pltpu.VMEM((n, 8, HEAD), f32),
        pltpu.VMEM((heads, HEAD, HEAD), f32),
        pltpu.VMEM((total, cols), bf),
        pltpu.VMEM((total, cols), bf),
        pltpu.VMEM((m - 1, rows, width), bf),
        pltpu.VMEM((m - 1, rows, width), bf),
        pltpu.VMEM((8, cols), f32),
        pltpu.VMEM((rows, width), f32),
        dma((m - 1,)),
        dma((m - 1,)),
        dma((NPROJ + 2, n)),
        dma((NPROJ + 2, n)),
        dma((NPROJ + 2, n)),
        dma((NPROJ + 2, n)),
        dma((NPROJ + 2, n)),
        dma((n,)),
        dma((n,)),
        dma((n,)),
        dma((n,)),
        dma,
        dma,
        dma((m - 1,)),
        dma((m - 1,)),
    ]
    return pl.pallas_call(
        functools.partial(kernel, sizes),
        out_shape=jax.ShapeDtypeStruct((rows, width), bf),
        in_specs=[pl.BlockSpec(memory_space=pltpu.VMEM)] * 16,
        out_specs=pl.BlockSpec(memory_space=pltpu.VMEM),
        scratch_shapes=scratch,
        compiler_params=pltpu.CompilerParams(
            collective_id=0, has_side_effects=True, vmem_limit_bytes=60 * 1024 * 1024
        ),
    )(tokens, gain[None, :], *args[2:12], log_decay, log_decay.T, cos2, sin2)


def solution(mesh):
    placed = (
        P(("grp", "sp", "tp"), None),
        P(),
        P("sp", "tp"),
        P("sp", "tp"),
        P("sp", "tp"),
        P("sp", "tp"),
        P("sp", "tp"),
        P("sp", "tp"),
        P("sp", "tp"),
        P(None, "tp"),
        P("tp", "sp"),
        P("tp", "sp"),
        P(("grp", "sp"), "tp"),
    )
    n, g, m = (mesh.shape[axis] for axis in ("sp", "grp", "tp"))
    fits = g == 2 and 2 <= n <= 4
    return jax.shard_map(
        functools.partial(fused, (n, g, m)) if fits else body, mesh=mesh, in_specs=placed, out_specs=P(("grp", "sp", "tp"), None), check_vma=False
    )
```

```python
import functools
import math

import jax
import jax.numpy as jnp
from jax import lax
from jax.experimental import pallas as pl
from jax.experimental.pallas import tpu as pltpu
from jax.sharding import PartitionSpec as P

HEAD = 128
CONV_K = 3
BLOCK = 128


EPSILON = 1e-06
ROTARY_BASE = 10000.0
HIGHEST_PRECISION = lax.Precision.HIGHEST


def prefix_2(x, axis, join, neutral):
    place = lax.axis_index(axis)
    gathered = jax.tree.map(
        lambda a, kind: lax.all_gather(a.astype(kind), axis), x, (jnp.bfloat16, jnp.bfloat16)
    )
    state = jax.tree.map(lambda a, e: jnp.zeros_like(a) + jnp.asarray(e, a.dtype), x, neutral)

    def one(turn, state):
        return join(
            state,
            jax.tree.map(
                lambda a, own: lax.dynamic_index_in_dim(a, turn, 0, False).astype(own.dtype),
                gathered,
                x,
            ),
        )

    return lax.fori_loop(0, place, one, state)


def shifted(x, axis, by):
    count = lax.axis_size(axis)
    pairs = [(i, i + by) for i in range(count) if 0 <= i + by < count]
    return lax.ppermute(x, axis, pairs)


def rotate(head_data, positions):
    half_width = head_data.shape[-1] // 2
    inv_freq = ROTARY_BASE ** (-jnp.arange(half_width, dtype=jnp.float32) / half_width)
    angles = positions[:, None] * inv_freq[None, :]
    cosine = jnp.cos(angles)[:, None, :]
    sine_part = jnp.sin(angles)[:, None, :]
    first_half = head_data[..., :half_width]
    second_half = head_data[..., half_width:]
    return jnp.concatenate(
        [
            first_half * cosine - second_half * sine_part,
            second_half * cosine + first_half * sine_part,
        ],
        axis=-1,
    )


def head_norm(head_data):
    return head_data * lax.rsqrt(jnp.mean(head_data * head_data, axis=-1, keepdims=True) + EPSILON)


def combine_states(earlier, later):
    return (earlier[0] * later[0], later[0][:, None, None] * earlier[1] + later[1])


def body(
    tokens,
    norm_gain,
    conv_outer_weight,
    conv_inner_weight,
    conv_input_weight,
    query_matrix,
    key_weight,
    value_weight,
    gate_weight,
    conv_taps,
    conv_out_weight,
    ret_out_weight,
    log_decay,
):
    values32 = tokens.astype(jnp.float32)
    normed = (
        values32
        * lax.rsqrt(jnp.mean(values32 * values32, axis=-1, keepdims=True) + EPSILON)
        * norm_gain.astype(jnp.float32)
    ).astype(jnp.bfloat16)
    gathered = lax.all_gather(normed, "tp", axis=0, tiled=True)
    row_total = gathered.shape[0]
    whole = (
        lax.all_gather(conv_outer_weight, "sp", axis=0, tiled=True),
        lax.all_gather(conv_inner_weight, "sp", axis=0, tiled=True),
        lax.all_gather(conv_input_weight, "sp", axis=0, tiled=True),
        lax.all_gather(query_matrix, "sp", axis=0, tiled=True),
        lax.all_gather(key_weight, "sp", axis=0, tiled=True),
        lax.all_gather(value_weight, "sp", axis=0, tiled=True),
        lax.all_gather(gate_weight, "sp", axis=0, tiled=True),
    )
    projected = tuple(
        (
            jnp.dot(gathered, weight, preferred_element_type=jnp.float32).astype(jnp.bfloat16)
            for weight in whole
        )
    )
    conv_outer, conv_inner, conv_input, query_proj, key_proj, value_proj, gate_proj = projected
    heads_here = query_proj.shape[1] // HEAD
    offset = (lax.axis_index("sp") * row_total).astype(jnp.float32)
    positions = offset + jnp.arange(row_total, dtype=jnp.float32)
    head_shape = (row_total, heads_here, HEAD)
    queries = rotate(query_proj.astype(jnp.float32).reshape(head_shape), positions)
    keys_rot = rotate(key_proj.astype(jnp.float32).reshape(head_shape), positions) * HEAD ** (-0.5)
    head_values = value_proj.astype(jnp.float32).reshape(head_shape)
    block_count = row_total // BLOCK
    block_shape = (block_count, BLOCK, heads_here, HEAD)
    query_blocks = queries.reshape(block_shape)
    key_blocks = keys_rot.reshape(block_shape)
    value_blocks = head_values.reshape(block_shape)
    log_blocks = log_decay.reshape(block_count, BLOCK, heads_here)
    offsets = jnp.arange(BLOCK, dtype=jnp.int32)
    causal_mask = offsets[:, None] >= offsets[None, :]
    lower_ones = causal_mask.astype(jnp.float32)
    cumulative = jnp.einsum("ij,njh->nih", lower_ones, log_blocks, precision=HIGHEST_PRECISION)
    block_end = cumulative[:, -1, :]
    mixed_in = conv_inner.astype(jnp.float32) * conv_input.astype(jnp.float32)
    rim = shifted(mixed_in[row_total - (CONV_K - 1) :], "sp", 1)
    extended = jnp.concatenate([rim, mixed_in], axis=0)
    taps = conv_taps.astype(jnp.float32)
    conv_out = jnp.zeros(mixed_in.shape, jnp.float32)
    for tap_index in range(CONV_K):
        conv_out = conv_out + taps[tap_index][None, :] * extended[tap_index : tap_index + row_total]
    conv_branch = (conv_outer.astype(jnp.float32) * conv_out).astype(jnp.bfloat16)
    weights = jnp.exp(block_end[:, None, :] - cumulative)
    increments = jnp.einsum(
        "njh,njhd,njhe->nhde", weights, key_blocks, value_blocks, precision=HIGHEST_PRECISION
    )

    def carry_on(carried, pieces):
        block_decay, increment = pieces
        return (block_decay[:, None, None] * carried + increment, carried)

    start_state = jnp.zeros((heads_here, HEAD, HEAD), jnp.float32)
    local_end, local_before = lax.scan(carry_on, start_state, (jnp.exp(block_end), increments))
    device_decay = jnp.exp(jnp.sum(block_end, axis=0))
    incoming = prefix_2(
        (device_decay, local_end),
        "sp",
        combine_states,
        (jnp.ones_like(device_decay), jnp.zeros_like(local_end)),
    )
    local_before, incoming_state = (local_before, incoming[1])
    spread = cumulative[:, :, None, :] - cumulative[:, None, :, :]
    grid_mask = causal_mask[None, :, :, None]
    decay_grid = jnp.where(grid_mask, jnp.exp(jnp.where(grid_mask, spread, 0.0)), 0.0)
    scores = (
        jnp.einsum("nihd,njhd->nijh", query_blocks, key_blocks, precision=HIGHEST_PRECISION)
        * decay_grid
    )
    within = jnp.einsum("nijh,njhe->nihe", scores, value_blocks, precision=HIGHEST_PRECISION)
    prefix = jnp.exp(jnp.cumsum(block_end, axis=0) - block_end)
    before = local_before + prefix[:, :, None, None] * incoming_state[None]
    across = jnp.einsum("nihd,nhde->nihe", query_blocks, before, precision=HIGHEST_PRECISION)
    across = across * jnp.exp(cumulative)[..., None]
    retained = (within + across).reshape(head_shape)
    ret_branch = (
        head_norm(retained).reshape(row_total, heads_here * HEAD)
        * jax.nn.silu(gate_proj.astype(jnp.float32))
    ).astype(jnp.bfloat16)
    conv_rows_weight, ret_rows_weight = (
        lax.all_gather(conv_out_weight, "sp", axis=1, tiled=True),
        lax.all_gather(ret_out_weight, "sp", axis=1, tiled=True),
    )
    return lax.psum_scatter(
        (
            jnp.dot(conv_branch, conv_rows_weight, preferred_element_type=jnp.float32)
            + jnp.dot(ret_branch, ret_rows_weight, preferred_element_type=jnp.float32)
        ).astype(jnp.bfloat16),
        "tp",
        scatter_dimension=0,
        tiled=True,
    )


MESH = pl.DeviceIdType.MESH
NPROJ = 7
ORDER = (3, 4, 5, 6, 1, 2, 0)
QUERY, KEY, VALUE, GATE, INNER, INPUT, OUTER = range(NPROJ)


def remote(src, dst, send, recv, axis, to):
    return pltpu.make_async_remote_copy(
        src_ref=src, dst_ref=dst, send_sem=send, recv_sem=recv, device_id={axis: to}, device_id_type=MESH
    )


def kernel(sizes, *refs):
    n, g, m = sizes
    tokens, gain, w0, w1, w2, w3, w4, w5, w6, taps, oc, orr, ldt, out = refs[:14]
    (raw, xn, gw, go, acc, ext, qr, kr, cum_s, cumt_s, cos2, sin2, kept_s, conv_s, lend, dec, instate, indec, sin_s, rb, cb, tail, own, swap) = refs[14:38]
    (tsend, trecv, rsend, lsend, zrecv, ysend, yrecv, ssend, srecv, dsend, drecv, csend, crecv, osend, orecv, xsend, xrecv, bsend, brecv, fsend, frecv) = refs[38:]
    weights = [(w0, w1, w2, w3, w4, w5, w6)[i] for i in ORDER]
    outs = (oc, orr)
    me = lax.axis_index("sp")
    grp = lax.axis_index("grp")
    mine = lax.axis_index("tp")
    rows, width = tokens.shape
    total = rows * m
    depth, cols = w0.shape
    half = depth // 2
    orows = oc.shape[0]
    ohalf = orows // 2
    ocols = oc.shape[1]
    heads = cols // HEAD
    other = 1 - grp

    barrier = pltpu.get_barrier_semaphore()
    for axis, count, at in (("sp", n, me), ("grp", g, grp), ("tp", m, mine)):
        for d in range(1, count):
            pl.semaphore_signal(barrier, inc=1, device_id={axis: lax.rem(at + d, count)}, device_id_type=MESH)
    pl.semaphore_wait(barrier, n + g + m - 3)

    twin = mine + 1 - 2 * lax.rem(mine, 2)
    far = lax.rem(mine + 2, m)
    far_twin = far + 1 - 2 * lax.rem(far, 2)

    def token_copy(k):
        src = raw.at[1] if k == 2 else tokens
        return remote(src, raw.at[k], tsend.at[k], trecv.at[k], "tp", far if k == 1 else twin)

    token_copy(1).start()
    token_copy(0).start()

    hs = pl.ds(pl.multiple_of(grp * half, half), half)
    ohs = pl.ds(pl.multiple_of(grp * ohalf, ohalf), ohalf)

    def slot(w, s, is_out):
        return go.at[mine, w, s, ohs] if is_out else gw.at[w, s, hs]

    def sem_at(w, is_out):
        return w + NPROJ if is_out else w

    def line_copy(w, s, is_out, right, src=None):
        dst = slot(w, s, is_out)
        k = sem_at(w, is_out)
        to = me + 1 if right else me - 1
        return remote(
            dst if src is None else src, dst, (rsend if right else lsend).at[k, s], zrecv.at[k, s], "sp", to
        )

    def pair_copy(w, s, is_out):
        part = slot(w, s, is_out)
        k = sem_at(w, is_out)
        return remote(part, part, ysend.at[k, s], yrecv.at[k, s], "grp", other)

    for w, is_out in [(0, True), (1, True)] + [(w, False) for w in range(NPROJ)]:
        src = outs[w].at[ohs] if is_out else weights[w].at[hs]

        @pl.when(me < n - 1)
        def _():
            line_copy(w, me, is_out, True, src).start()

        @pl.when(me > 0)
        def _():
            line_copy(w, me, is_out, False, src).start()

    def far_copy(w, s, src=None):
        part = go.at[mine, w, s]
        return remote(part if src is None else src, part, xsend.at[w, s], xrecv.at[w, s], "tp", far)

    def twin_copy(w, s, src=None):
        part = go.at[mine, w, s]
        return remote(part if src is None else src, part, bsend.at[w, s], brecv.at[w, s], "tp", twin)

    def relay_copy(w, s):
        part = go.at[far, w, s]
        return remote(part, part, fsend.at[w, s], frecv.at[w, s], "tp", twin)

    for w in range(2):
        far_copy(w, me, outs[w]).start()
        twin_copy(w, me, outs[w]).start()

    below = lax.broadcasted_iota(jnp.int32, (total, total), 0) >= lax.broadcasted_iota(jnp.int32, (total, total), 1)

    def decay_sums():
        lower = below.astype(jnp.float32)
        nt = (((1,), (1,)), ((), ()))
        cum_s[...] = lax.dot_general(lower, ldt[...], nt, precision=HIGHEST_PRECISION, preferred_element_type=jnp.float32)
        cumt_s[...] = lax.dot_general(ldt[...], lower, nt, precision=HIGHEST_PRECISION, preferred_element_type=jnp.float32)

    def tables():
        half_width = HEAD // 2
        lane = lax.broadcasted_iota(jnp.int32, (total, HEAD), 1)
        first = lane < half_width
        index = jnp.where(first, lane, lane - half_width).astype(jnp.float32)
        place = (lax.broadcasted_iota(jnp.int32, (total, HEAD), 0) + me * total).astype(jnp.float32)
        angle = place * jnp.exp(index * (-math.log(ROTARY_BASE) / half_width))
        cos2[...] = jnp.cos(angle)
        sine = jnp.sin(angle)
        sin2[...] = jnp.where(first, -sine, sine)

    step_rows = 16
    scale = gain[...].astype(jnp.float32)[None, :]

    def normalise(source, block):
        def one(i, carry):
            at = pl.multiple_of(i * step_rows, step_rows)
            v = source[pl.ds(at, step_rows), :].astype(jnp.float32)
            r = lax.rsqrt(jnp.mean(v * v, axis=-1, keepdims=True) + EPSILON)
            y = (v * r * scale).astype(jnp.bfloat16)
            to = pl.ds(pl.multiple_of(block * rows + at, step_rows), step_rows)
            for s in range(n):
                xn[s, to, :] = y[:, s * depth : (s + 1) * depth]
            return carry

        lax.fori_loop(0, rows // step_rows, one, 0)

    def forward(w, is_out, d):
        @pl.when(me >= d)
        def _():
            s = me - d
            line_copy(w, s, is_out, True).wait_recv()

            @pl.when(me < n - 1)
            def _():
                line_copy(w, s, is_out, True).start()

            pair_copy(w, s, is_out).start()

        @pl.when(me + d < n)
        def _():
            s = me + d
            line_copy(w, s, is_out, False).wait_recv()

            @pl.when(me > 0)
            def _():
                line_copy(w, s, is_out, False).start()

            pair_copy(w, s, is_out).start()

    def other_wait(w, s, is_out):
        theirs = (
            go.at[mine, w, s, pl.ds(pl.multiple_of(other * ohalf, ohalf), ohalf)]
            if is_out
            else gw.at[w, s, pl.ds(pl.multiple_of(other * half, half), half)]
        )
        k = sem_at(w, is_out)
        remote(theirs, theirs, ysend.at[k, s], yrecv.at[k, s], "grp", other).wait_recv()

    def consume(w, d):
        @pl.when(me >= d)
        def _():
            s = me - d
            other_wait(w, s, False)
            acc[w] += jnp.dot(xn[s], gw[w, s], preferred_element_type=jnp.float32)

        @pl.when(me + d < n)
        def _():
            s = me + d
            other_wait(w, s, False)
            acc[w] += jnp.dot(xn[s], gw[w, s], preferred_element_type=jnp.float32)

    def block_one():
        token_copy(0).wait_recv()
        normalise(raw.at[0], twin)

    def block_two():
        token_copy(1).wait_recv()
        token_copy(2).start()
        normalise(raw.at[1], far)

    def block_three():
        token_copy(2).wait_recv()
        normalise(raw.at[2], far_twin)

    def own_dots(which):
        for w in which:
            acc[w] = jnp.dot(xn[me], weights[w][...], preferred_element_type=jnp.float32)

    def at_distance(d, act):
        @pl.when(me >= d)
        def _():
            act(me - d)

        @pl.when(me + d < n)
        def _():
            act(me + d)

    def share(d):
        def act(s):
            for w in range(2):
                other_wait(w, s, True)
                far_copy(w, s).start()
                twin_copy(w, s).start()

        at_distance(d, act)

    def relay(d):
        def act(s):
            for w in range(2):
                far_copy(w, s).wait_recv()
                relay_copy(w, s).start()

        at_distance(d, act)

    def keep_own():
        for w in range(2):
            go[mine, w, me] = outs[w][...]

    def relay_own():
        for w in range(2):
            far_copy(w, me).wait_recv()
            relay_copy(w, me).start()

    def own_low():
        own_dots(range(4))

    def own_high():
        own_dots(range(4, NPROJ))

    jobs = [decay_sums, tables, lambda: normalise(tokens, mine), block_one, block_two, block_three, own_low, own_high, keep_own]
    forward(0, True, 1)
    jobs[0]()
    forward(1, True, 1)
    jobs[1]()
    for w in range(NPROJ):
        forward(w, False, 1)
        jobs[w + 2]()
    share(1)
    relay_own()

    def steps(d, lo, hi):
        def one(i, carry):
            forward(i, False, d)
            consume(i, d - 1)
            return carry

        lax.fori_loop(lo, hi, one, 0)

    def finish(lo, hi):
        if n < 3:
            return

        def one(i, carry):
            consume(i, n - 1)
            return carry

        lax.fori_loop(lo, hi, one, 0)

    for d in range(2, n):
        forward(0, True, d)
        forward(1, True, d)
        steps(d, 0, 3)
        share(d)
        relay(d - 1)
        if d < n - 1:
            steps(d, 3, NPROJ)
    finish(0, 3)

    def projected(w, h=None):
        part = acc[w] if h is None else acc[w, :, h * HEAD : (h + 1) * HEAD]
        return part.astype(jnp.bfloat16).astype(jnp.float32)

    def state_copy(d):
        return remote(lend, instate.at[me], ssend.at[d - 1], srecv.at[me], "sp", me + d)

    def decay_copy(d):
        return remote(dec, indec.at[me], dsend.at[d - 1], drecv.at[me], "sp", me + d)

    dec[...] = jnp.zeros_like(dec)
    for h in range(heads):
        k = projected(KEY, h)
        k = (k * cos2[...] + pltpu.roll(k, HEAD // 2, 1) * sin2[...]) * HEAD ** (-0.5)
        kr[h] = k.astype(jnp.bfloat16)
        q = projected(QUERY, h)
        qr[h] = (q * cos2[...] + pltpu.roll(q, HEAD // 2, 1) * sin2[...]).astype(jnp.bfloat16)
        c = cum_s[:, h : h + 1]
        end = cum_s[total - 1 : total, h : h + 1]
        kw = (k * jnp.exp(end - c)).astype(jnp.bfloat16)
        vals = acc[VALUE, :, h * HEAD : (h + 1) * HEAD].astype(jnp.bfloat16)
        lend[h] = lax.dot_general(kw, vals, (((0,), (0,)), ((), ())), preferred_element_type=jnp.float32).astype(jnp.bfloat16)
        dec[h : h + 1, :] = jnp.broadcast_to(end, (1, HEAD))
    for d in range(1, n):

        @pl.when(me + d < n)
        def _():
            state_copy(d).start()
            decay_copy(d).start()

    values = [acc[VALUE, :, h * HEAD : (h + 1) * HEAD].astype(jnp.bfloat16) for h in range(heads)]
    steps(n - 1, 3, 4)
    for h in range(heads):
        c = cum_s[:, h : h + 1]
        spread = c - cumt_s[h : h + 1, :]
        grid = jnp.where(below, jnp.exp(jnp.where(below, spread, 0.0)), 0.0)
        scores = lax.dot_general(qr[h], kr[h], (((1,), (1,)), ((), ())), preferred_element_type=jnp.float32) * grid
        kept_s[h] = jnp.dot(scores.astype(jnp.bfloat16), values[h], preferred_element_type=jnp.float32)
        steps(n - 1, 4 + h, 5 + h) if h < 2 else None
    steps(n - 1, min(4 + heads, 6), NPROJ)
    relay(n - 1)
    finish(3, 4)

    sin_s[...] = jnp.zeros_like(sin_s)
    for s in range(n - 1):

        @pl.when(me > s)
        def _():
            remote(lend, instate.at[s], ssend.at[0], srecv.at[s], "sp", s).wait_recv()
            remote(dec, indec.at[s], dsend.at[0], drecv.at[s], "sp", s).wait_recv()
            for h in range(heads):
                sin_s[h] = jnp.exp(indec[s, h : h + 1, :]) * sin_s[h] + instate[s, h].astype(jnp.float32)

    for h in range(heads):
        c = cum_s[:, h : h + 1]
        kept = kept_s[h]
        kept += jnp.dot(qr[h], sin_s[h].astype(jnp.bfloat16), preferred_element_type=jnp.float32) * jnp.exp(c)
        gate = projected(GATE, h)
        normed = kept * lax.rsqrt(jnp.mean(kept * kept, axis=-1, keepdims=True) + EPSILON)
        rb[:, h * HEAD : (h + 1) * HEAD] = (normed * (gate / (1.0 + jnp.exp(-gate)))).astype(jnp.bfloat16)

    def block(ref, to):
        return ref.at[pl.ds(pl.multiple_of(to * rows, rows), rows)]

    def branch_copy(kind, k):
        to = (twin, far, far_twin)[k]
        return remote(block((cb, rb)[kind], to), swap.at[kind, k], osend.at[kind, k], orecv.at[kind, k], "tp", to)

    for k in (1, 2, 0):
        branch_copy(1, k).start()

    finish(INNER, INPUT + 1)
    mixed_in = projected(INNER) * projected(INPUT)
    ext[8:, :] = mixed_in
    tail[...] = mixed_in[total - 8 :, :]

    def rim_copy():
        return remote(tail, ext.at[0:8], csend, crecv, "sp", me + 1)

    @pl.when(me < n - 1)
    def _():
        rim_copy().start()

    for d in range(1, n):
        at_distance(d, lambda s: [twin_copy(w, s).wait_recv() for w in range(2)])
        at_distance(d, lambda s: [relay_copy(w, s).wait_recv() for w in range(2)])
    for w in range(2):
        twin_copy(w, me).wait_recv()
        relay_copy(w, me).wait_recv()

    owners = (twin, far, far_twin)

    def add_branch(kind):
        at = pl.ds(pl.multiple_of(mine * rows, rows), rows)
        for k in range(m - 1):
            branch_copy(kind, k).wait_recv()
        parts = [(cb, rb)[kind][at, :]] + [swap[kind, k] for k in range(m - 1)]
        for s in range(n):
            to = slice(s * ocols, (s + 1) * ocols)
            value = jnp.dot(parts[0], go[mine, kind, s], preferred_element_type=jnp.float32)
            for k in range(m - 1):
                value += jnp.dot(parts[k + 1], go[owners[k], kind, s], preferred_element_type=jnp.float32)
            if kind == 1:
                own[:, to] = value
            else:
                out[:, to] = (own[:, to] + value).astype(jnp.bfloat16)

    add_branch(1)

    @pl.when(me > 0)
    def _():
        remote(tail, ext.at[0:8], csend, crecv, "sp", me - 1).wait_recv()

    @pl.when(me == 0)
    def _():
        ext[0:8, :] = jnp.zeros((8, cols), jnp.float32)

    t = taps[...].astype(jnp.float32)
    conv = jnp.zeros((total, cols), jnp.float32)
    for j in range(CONV_K):
        lo = 8 - (CONV_K - 1) + j
        conv = conv + t[j : j + 1, :] * ext[lo : lo + total, :]
    conv_s[...] = conv
    finish(OUTER, OUTER + 1)
    cb[...] = (projected(OUTER) * conv_s[...]).astype(jnp.bfloat16)
    for k in (1, 2, 0):
        branch_copy(0, k).start()
    add_branch(0)

    for k in range(m - 1):
        token_copy(k).wait_send()
        for kind in range(2):
            branch_copy(kind, k).wait_send()
    for w in range(2):
        for s in range(n):
            far_copy(w, s).wait_send()
            twin_copy(w, s).wait_send()
            relay_copy(w, s).wait_send()
    for d in range(1, n):

        @pl.when(me + d < n)
        def _():
            state_copy(d).wait_send()
            decay_copy(d).wait_send()

    @pl.when(me < n - 1)
    def _():
        rim_copy().wait_send()

    for is_out, count in ((True, 2), (False, NPROJ)):

        def drain(w, carry):
            for s in range(n):

                @pl.when((s <= me) & (me < n - 1))
                def _():
                    line_copy(w, s, is_out, True).wait_send()

                @pl.when((s >= me) & (me > 0))
                def _():
                    line_copy(w, s, is_out, False).wait_send()

                @pl.when(me != s)
                def _():
                    pair_copy(w, s, is_out).wait_send()

            return carry

        lax.fori_loop(0, count, drain, 0)


def fused(sizes, *args):
    n, g, m = sizes
    tokens, gain, w0 = args[0], args[1], args[2]
    log_decay = args[12]
    rows, width = tokens.shape
    depth, cols = w0.shape
    orows, ocols = args[10].shape
    total = rows * m
    heads = cols // HEAD
    bf, f32 = jnp.bfloat16, jnp.float32
    dma = pltpu.SemaphoreType.DMA
    scratch = [
        pltpu.VMEM((m - 1, rows, width), bf),
        pltpu.VMEM((n, total, depth), bf),
        pltpu.VMEM((NPROJ, n, depth, cols), bf),
        pltpu.VMEM((m, 2, n, orows, ocols), bf),
        pltpu.VMEM((NPROJ, total, cols), f32),
        pltpu.VMEM((total + 8, cols), f32),
        pltpu.VMEM((heads, total, HEAD), bf),
        pltpu.VMEM((heads, total, HEAD), bf),
        pltpu.VMEM((total, heads), f32),
        pltpu.VMEM((heads, total), f32),
        pltpu.VMEM((total, HEAD), f32),
        pltpu.VMEM((total, HEAD), f32),
        pltpu.VMEM((heads, total, HEAD), f32),
        pltpu.VMEM((total, cols), f32),
        pltpu.VMEM((heads, HEAD, HEAD), bf),
        pltpu.VMEM((8, HEAD), f32),
        pltpu.VMEM((n, heads, HEAD, HEAD), bf),
        pltpu.VMEM((n, 8, HEAD), f32),
        pltpu.VMEM((heads, HEAD, HEAD), f32),
        pltpu.VMEM((total, cols), bf),
        pltpu.VMEM((total, cols), bf),
        pltpu.VMEM((8, cols), f32),
        pltpu.VMEM((rows, width), f32),
        pltpu.VMEM((2, m - 1, rows, cols), bf),
        dma((m - 1,)),
        dma((m - 1,)),
        dma((NPROJ + 2, n)),
        dma((NPROJ + 2, n)),
        dma((NPROJ + 2, n)),
        dma((NPROJ + 2, n)),
        dma((NPROJ + 2, n)),
        dma((n,)),
        dma((n,)),
        dma((n,)),
        dma((n,)),
        dma,
        dma,
        dma((2, m - 1)),
        dma((2, m - 1)),
    ] + [dma((2, n))] * 6
    return pl.pallas_call(
        functools.partial(kernel, sizes),
        out_shape=jax.ShapeDtypeStruct((rows, width), bf),
        in_specs=[pl.BlockSpec(memory_space=pltpu.VMEM)] * 13,
        out_specs=pl.BlockSpec(memory_space=pltpu.VMEM),
        scratch_shapes=scratch,
        compiler_params=pltpu.CompilerParams(
            collective_id=0, has_side_effects=True, vmem_limit_bytes=60 * 1024 * 1024
        ),
    )(tokens, gain, *args[2:12], log_decay.T)


def solution(mesh):
    placed = (
        P(("grp", "sp", "tp"), None),
        P(),
        P("sp", "tp"),
        P("sp", "tp"),
        P("sp", "tp"),
        P("sp", "tp"),
        P("sp", "tp"),
        P("sp", "tp"),
        P("sp", "tp"),
        P(None, "tp"),
        P("tp", "sp"),
        P("tp", "sp"),
        P(("grp", "sp"), "tp"),
    )
    n, g, m = (mesh.shape[axis] for axis in ("sp", "grp", "tp"))
    fits = g == 2 and m == 4 and 3 <= n <= 4
    return jax.shard_map(
        functools.partial(fused, (n, g, m)) if fits else body, mesh=mesh, in_specs=placed, out_specs=P(("grp", "sp", "tp"), None), check_vma=False
    )
```

```python
import functools
import math

import jax
import jax.numpy as jnp
from jax import lax
from jax.experimental import pallas as pl
from jax.experimental.pallas import tpu as pltpu
from jax.sharding import PartitionSpec as P

HEAD = 128
CONV_K = 3
BLOCK = 128


EPSILON = 1e-06
ROTARY_BASE = 10000.0
HIGHEST_PRECISION = lax.Precision.HIGHEST


def prefix_2(x, axis, join, neutral):
    place = lax.axis_index(axis)
    gathered = jax.tree.map(
        lambda a, kind: lax.all_gather(a.astype(kind), axis), x, (jnp.bfloat16, jnp.bfloat16)
    )
    state = jax.tree.map(lambda a, e: jnp.zeros_like(a) + jnp.asarray(e, a.dtype), x, neutral)

    def one(turn, state):
        return join(
            state,
            jax.tree.map(
                lambda a, own: lax.dynamic_index_in_dim(a, turn, 0, False).astype(own.dtype),
                gathered,
                x,
            ),
        )

    return lax.fori_loop(0, place, one, state)


def shifted(x, axis, by):
    count = lax.axis_size(axis)
    pairs = [(i, i + by) for i in range(count) if 0 <= i + by < count]
    return lax.ppermute(x, axis, pairs)


def rotate(head_data, positions):
    half_width = head_data.shape[-1] // 2
    inv_freq = ROTARY_BASE ** (-jnp.arange(half_width, dtype=jnp.float32) / half_width)
    angles = positions[:, None] * inv_freq[None, :]
    cosine = jnp.cos(angles)[:, None, :]
    sine_part = jnp.sin(angles)[:, None, :]
    first_half = head_data[..., :half_width]
    second_half = head_data[..., half_width:]
    return jnp.concatenate(
        [
            first_half * cosine - second_half * sine_part,
            second_half * cosine + first_half * sine_part,
        ],
        axis=-1,
    )


def head_norm(head_data):
    return head_data * lax.rsqrt(jnp.mean(head_data * head_data, axis=-1, keepdims=True) + EPSILON)


def combine_states(earlier, later):
    return (earlier[0] * later[0], later[0][:, None, None] * earlier[1] + later[1])


def body(
    tokens,
    norm_gain,
    conv_outer_weight,
    conv_inner_weight,
    conv_input_weight,
    query_matrix,
    key_weight,
    value_weight,
    gate_weight,
    conv_taps,
    conv_out_weight,
    ret_out_weight,
    log_decay,
):
    values32 = tokens.astype(jnp.float32)
    normed = (
        values32
        * lax.rsqrt(jnp.mean(values32 * values32, axis=-1, keepdims=True) + EPSILON)
        * norm_gain.astype(jnp.float32)
    ).astype(jnp.bfloat16)
    gathered = lax.all_gather(normed, "tp", axis=0, tiled=True)
    row_total = gathered.shape[0]
    whole = (
        lax.all_gather(conv_outer_weight, "sp", axis=0, tiled=True),
        lax.all_gather(conv_inner_weight, "sp", axis=0, tiled=True),
        lax.all_gather(conv_input_weight, "sp", axis=0, tiled=True),
        lax.all_gather(query_matrix, "sp", axis=0, tiled=True),
        lax.all_gather(key_weight, "sp", axis=0, tiled=True),
        lax.all_gather(value_weight, "sp", axis=0, tiled=True),
        lax.all_gather(gate_weight, "sp", axis=0, tiled=True),
    )
    projected = tuple(
        (
            jnp.dot(gathered, weight, preferred_element_type=jnp.float32).astype(jnp.bfloat16)
            for weight in whole
        )
    )
    conv_outer, conv_inner, conv_input, query_proj, key_proj, value_proj, gate_proj = projected
    heads_here = query_proj.shape[1] // HEAD
    offset = (lax.axis_index("sp") * row_total).astype(jnp.float32)
    positions = offset + jnp.arange(row_total, dtype=jnp.float32)
    head_shape = (row_total, heads_here, HEAD)
    queries = rotate(query_proj.astype(jnp.float32).reshape(head_shape), positions)
    keys_rot = rotate(key_proj.astype(jnp.float32).reshape(head_shape), positions) * HEAD ** (-0.5)
    head_values = value_proj.astype(jnp.float32).reshape(head_shape)
    block_count = row_total // BLOCK
    block_shape = (block_count, BLOCK, heads_here, HEAD)
    query_blocks = queries.reshape(block_shape)
    key_blocks = keys_rot.reshape(block_shape)
    value_blocks = head_values.reshape(block_shape)
    log_blocks = log_decay.reshape(block_count, BLOCK, heads_here)
    offsets = jnp.arange(BLOCK, dtype=jnp.int32)
    causal_mask = offsets[:, None] >= offsets[None, :]
    lower_ones = causal_mask.astype(jnp.float32)
    cumulative = jnp.einsum("ij,njh->nih", lower_ones, log_blocks, precision=HIGHEST_PRECISION)
    block_end = cumulative[:, -1, :]
    mixed_in = conv_inner.astype(jnp.float32) * conv_input.astype(jnp.float32)
    rim = shifted(mixed_in[row_total - (CONV_K - 1) :], "sp", 1)
    extended = jnp.concatenate([rim, mixed_in], axis=0)
    taps = conv_taps.astype(jnp.float32)
    conv_out = jnp.zeros(mixed_in.shape, jnp.float32)
    for tap_index in range(CONV_K):
        conv_out = conv_out + taps[tap_index][None, :] * extended[tap_index : tap_index + row_total]
    conv_branch = (conv_outer.astype(jnp.float32) * conv_out).astype(jnp.bfloat16)
    weights = jnp.exp(block_end[:, None, :] - cumulative)
    increments = jnp.einsum(
        "njh,njhd,njhe->nhde", weights, key_blocks, value_blocks, precision=HIGHEST_PRECISION
    )

    def carry_on(carried, pieces):
        block_decay, increment = pieces
        return (block_decay[:, None, None] * carried + increment, carried)

    start_state = jnp.zeros((heads_here, HEAD, HEAD), jnp.float32)
    local_end, local_before = lax.scan(carry_on, start_state, (jnp.exp(block_end), increments))
    device_decay = jnp.exp(jnp.sum(block_end, axis=0))
    incoming = prefix_2(
        (device_decay, local_end),
        "sp",
        combine_states,
        (jnp.ones_like(device_decay), jnp.zeros_like(local_end)),
    )
    local_before, incoming_state = (local_before, incoming[1])
    spread = cumulative[:, :, None, :] - cumulative[:, None, :, :]
    grid_mask = causal_mask[None, :, :, None]
    decay_grid = jnp.where(grid_mask, jnp.exp(jnp.where(grid_mask, spread, 0.0)), 0.0)
    scores = (
        jnp.einsum("nihd,njhd->nijh", query_blocks, key_blocks, precision=HIGHEST_PRECISION)
        * decay_grid
    )
    within = jnp.einsum("nijh,njhe->nihe", scores, value_blocks, precision=HIGHEST_PRECISION)
    prefix = jnp.exp(jnp.cumsum(block_end, axis=0) - block_end)
    before = local_before + prefix[:, :, None, None] * incoming_state[None]
    across = jnp.einsum("nihd,nhde->nihe", query_blocks, before, precision=HIGHEST_PRECISION)
    across = across * jnp.exp(cumulative)[..., None]
    retained = (within + across).reshape(head_shape)
    ret_branch = (
        head_norm(retained).reshape(row_total, heads_here * HEAD)
        * jax.nn.silu(gate_proj.astype(jnp.float32))
    ).astype(jnp.bfloat16)
    conv_rows_weight, ret_rows_weight = (
        lax.all_gather(conv_out_weight, "sp", axis=1, tiled=True),
        lax.all_gather(ret_out_weight, "sp", axis=1, tiled=True),
    )
    return lax.psum_scatter(
        (
            jnp.dot(conv_branch, conv_rows_weight, preferred_element_type=jnp.float32)
            + jnp.dot(ret_branch, ret_rows_weight, preferred_element_type=jnp.float32)
        ).astype(jnp.bfloat16),
        "tp",
        scatter_dimension=0,
        tiled=True,
    )


MESH = pl.DeviceIdType.MESH
NPROJ = 7
ORDER = (3, 4, 5, 6, 1, 2, 0)
QUERY, KEY, VALUE, GATE, INNER, INPUT, OUTER = range(NPROJ)


def remote(src, dst, send, recv, axis, to):
    return pltpu.make_async_remote_copy(
        src_ref=src, dst_ref=dst, send_sem=send, recv_sem=recv, device_id={axis: to}, device_id_type=MESH
    )


def kernel(sizes, *refs):
    n, g, m = sizes
    tokens, gain, w0, w1, w2, w3, w4, w5, w6, taps, oc, orr, ldt, out = refs[:14]
    (raw, xn, gw, go, acc, ext, qr, kr, cum_s, cumt_s, cos2, sin2, kept_s, conv_s, lend, dec, instate, indec, sin_s, rb, cb, tail, own, swap) = refs[14:38]
    (tsend, trecv, rsend, lsend, zrecv, ysend, yrecv, ssend, srecv, dsend, drecv, csend, crecv, osend, orecv, xsend, xrecv, bsend, brecv, fsend, frecv) = refs[38:]
    weights = [(w0, w1, w2, w3, w4, w5, w6)[i] for i in ORDER]
    outs = (oc, orr)
    me = lax.axis_index("sp")
    grp = lax.axis_index("grp")
    mine = lax.axis_index("tp")
    rows, width = tokens.shape
    total = rows * m
    depth, cols = w0.shape
    half = depth // 2
    orows = oc.shape[0]
    ohalf = orows // 2
    ocols = oc.shape[1]
    heads = cols // HEAD
    other = 1 - grp

    barrier = pltpu.get_barrier_semaphore()
    for axis, count, at in (("sp", n, me), ("grp", g, grp), ("tp", m, mine)):
        for d in range(1, count):
            pl.semaphore_signal(barrier, inc=1, device_id={axis: lax.rem(at + d, count)}, device_id_type=MESH)
    pl.semaphore_wait(barrier, n + g + m - 3)

    twin = mine + 1 - 2 * lax.rem(mine, 2)
    far = lax.rem(mine + 2, m)
    far_twin = far + 1 - 2 * lax.rem(far, 2)

    def token_copy(k):
        src = raw.at[1] if k == 2 else tokens
        return remote(src, raw.at[k], tsend.at[k], trecv.at[k], "tp", far if k == 1 else twin)

    token_copy(1).start()
    token_copy(0).start()

    hs = pl.ds(pl.multiple_of(grp * half, half), half)
    ohs = pl.ds(pl.multiple_of(grp * ohalf, ohalf), ohalf)

    def slot(w, s, is_out):
        return go.at[mine, w, s, ohs] if is_out else gw.at[w, s, hs]

    def sem_at(w, is_out):
        return w + NPROJ if is_out else w

    def line_copy(w, s, is_out, right, src=None):
        dst = slot(w, s, is_out)
        k = sem_at(w, is_out)
        to = me + 1 if right else me - 1
        return remote(
            dst if src is None else src, dst, (rsend if right else lsend).at[k, s], zrecv.at[k, s], "sp", to
        )

    def pair_copy(w, s, is_out):
        part = slot(w, s, is_out)
        k = sem_at(w, is_out)
        return remote(part, part, ysend.at[k, s], yrecv.at[k, s], "grp", other)

    for w, is_out in [(0, True), (1, True)] + [(w, False) for w in range(NPROJ)]:
        src = outs[w].at[ohs] if is_out else weights[w].at[hs]

        @pl.when(me < n - 1)
        def _():
            line_copy(w, me, is_out, True, src).start()

        @pl.when(me > 0)
        def _():
            line_copy(w, me, is_out, False, src).start()

    def far_copy(w, s, src=None):
        part = go.at[mine, w, s]
        return remote(part if src is None else src, part, xsend.at[w, s], xrecv.at[w, s], "tp", far)

    def twin_copy(w, s, src=None):
        part = go.at[mine, w, s]
        return remote(part if src is None else src, part, bsend.at[w, s], brecv.at[w, s], "tp", twin)

    def relay_copy(w, s):
        part = go.at[far, w, s]
        return remote(part, part, fsend.at[w, s], frecv.at[w, s], "tp", twin)

    for w in range(2):
        far_copy(w, me, outs[w]).start()
        twin_copy(w, me, outs[w]).start()

    below = lax.broadcasted_iota(jnp.int32, (total, total), 0) >= lax.broadcasted_iota(jnp.int32, (total, total), 1)

    def decay_sums():
        lower = below.astype(jnp.float32)
        nt = (((1,), (1,)), ((), ()))
        cum_s[...] = lax.dot_general(lower, ldt[...], nt, precision=HIGHEST_PRECISION, preferred_element_type=jnp.float32)
        cumt_s[...] = lax.dot_general(ldt[...], lower, nt, precision=HIGHEST_PRECISION, preferred_element_type=jnp.float32)

    pieces = NPROJ + 1
    piece_rows = total // pieces

    def tables(i):
        half_width = HEAD // 2
        lane = lax.broadcasted_iota(jnp.int32, (piece_rows, HEAD), 1)
        first = lane < half_width
        index = jnp.where(first, lane, lane - half_width).astype(jnp.float32)
        start = i * piece_rows
        place = (lax.broadcasted_iota(jnp.int32, (piece_rows, HEAD), 0) + me * total + start).astype(jnp.float32)
        angle = place * jnp.exp(index * (-math.log(ROTARY_BASE) / half_width))
        at = pl.ds(start if isinstance(start, int) else pl.multiple_of(start, piece_rows), piece_rows)
        cos2[at, :] = jnp.cos(angle)
        sine = jnp.sin(angle)
        sin2[at, :] = jnp.where(first, -sine, sine)

    step_rows = 16
    scale = gain[...].astype(jnp.float32)[None, :]

    def normalise(source, block):
        def one(i, carry):
            at = pl.multiple_of(i * step_rows, step_rows)
            v = source[pl.ds(at, step_rows), :].astype(jnp.float32)
            r = lax.rsqrt(jnp.mean(v * v, axis=-1, keepdims=True) + EPSILON)
            y = (v * r * scale).astype(jnp.bfloat16)
            to = pl.ds(pl.multiple_of(block * rows + at, step_rows), step_rows)
            for s in range(n):
                xn[s, to, :] = y[:, s * depth : (s + 1) * depth]
            return carry

        lax.fori_loop(0, rows // step_rows, one, 0)

    def forward(w, is_out, d):
        @pl.when(me >= d)
        def _():
            s = me - d
            line_copy(w, s, is_out, True).wait_recv()

            @pl.when(me < n - 1)
            def _():
                line_copy(w, s, is_out, True).start()

            pair_copy(w, s, is_out).start()

        @pl.when(me + d < n)
        def _():
            s = me + d
            line_copy(w, s, is_out, False).wait_recv()

            @pl.when(me > 0)
            def _():
                line_copy(w, s, is_out, False).start()

            pair_copy(w, s, is_out).start()

    def other_wait(w, s, is_out):
        theirs = (
            go.at[mine, w, s, pl.ds(pl.multiple_of(other * ohalf, ohalf), ohalf)]
            if is_out
            else gw.at[w, s, pl.ds(pl.multiple_of(other * half, half), half)]
        )
        k = sem_at(w, is_out)
        remote(theirs, theirs, ysend.at[k, s], yrecv.at[k, s], "grp", other).wait_recv()

    def consume(w, d):
        @pl.when(me >= d)
        def _():
            s = me - d
            other_wait(w, s, False)
            acc[w] += jnp.dot(xn[s], gw[w, s], preferred_element_type=jnp.float32)

        @pl.when(me + d < n)
        def _():
            s = me + d
            other_wait(w, s, False)
            acc[w] += jnp.dot(xn[s], gw[w, s], preferred_element_type=jnp.float32)

    def block_one():
        token_copy(0).wait_recv()
        normalise(raw.at[0], twin)

    def block_two():
        token_copy(1).wait_recv()
        token_copy(2).start()
        normalise(raw.at[1], far)

    def block_three():
        token_copy(2).wait_recv()
        normalise(raw.at[2], far_twin)

    def own_dots(which):
        for w in which:
            acc[w] = jnp.dot(xn[me], weights[w][...], preferred_element_type=jnp.float32)

    def at_distance(d, act):
        @pl.when(me >= d)
        def _():
            act(me - d)

        @pl.when(me + d < n)
        def _():
            act(me + d)

    def share(d):
        def act(s):
            for w in range(2):
                other_wait(w, s, True)
                far_copy(w, s).start()
                twin_copy(w, s).start()

        at_distance(d, act)

    def relay(d):
        def act(s):
            for w in range(2):
                far_copy(w, s).wait_recv()
                relay_copy(w, s).start()

        at_distance(d, act)

    def keep_own():
        for w in range(2):
            go[mine, w, me] = outs[w][...]

    def relay_own():
        for w in range(2):
            far_copy(w, me).wait_recv()
            relay_copy(w, me).start()

    def own_low():
        own_dots(range(4))

    def own_high():
        own_dots(range(4, NPROJ))

    jobs = [lambda: normalise(tokens, mine), block_one, block_two, block_three, own_low, own_high, keep_own]
    decay_sums()
    forward(0, True, 1)
    forward(1, True, 1)
    for w in range(NPROJ):
        forward(w, False, 1)
        jobs[w]()
    share(1)
    relay_own()
    tables(NPROJ)

    def steps(d, lo, hi):
        def one(i, carry):
            forward(i, False, d)
            consume(i, d - 1)
            if d == 2:
                tables(i)
            return carry

        lax.fori_loop(lo, hi, one, 0)

    def finish(lo, hi):
        if n < 3:
            return

        def one(i, carry):
            consume(i, n - 1)
            return carry

        lax.fori_loop(lo, hi, one, 0)

    for d in range(2, n):
        forward(0, True, d)
        forward(1, True, d)
        steps(d, 0, 3)
        share(d)
        relay(d - 1)
        if d < n - 1:
            steps(d, 3, NPROJ)
    steps(n - 1, 3, 4)
    finish(0, 3)

    def projected(w, h=None):
        part = acc[w] if h is None else acc[w, :, h * HEAD : (h + 1) * HEAD]
        return part.astype(jnp.bfloat16).astype(jnp.float32)

    def state_copy(d):
        return remote(lend, instate.at[me], ssend.at[d - 1], srecv.at[me], "sp", me + d)

    def decay_copy(d):
        return remote(dec, indec.at[me], dsend.at[d - 1], drecv.at[me], "sp", me + d)

    dec[...] = jnp.zeros_like(dec)
    for h in range(heads):
        k = projected(KEY, h)
        k = (k * cos2[...] + pltpu.roll(k, HEAD // 2, 1) * sin2[...]) * HEAD ** (-0.5)
        kr[h] = k.astype(jnp.bfloat16)
        q = projected(QUERY, h)
        qr[h] = (q * cos2[...] + pltpu.roll(q, HEAD // 2, 1) * sin2[...]).astype(jnp.bfloat16)
        c = cum_s[:, h : h + 1]
        end = cum_s[total - 1 : total, h : h + 1]
        kw = (k * jnp.exp(end - c)).astype(jnp.bfloat16)
        vals = acc[VALUE, :, h * HEAD : (h + 1) * HEAD].astype(jnp.bfloat16)
        lend[h] = lax.dot_general(kw, vals, (((0,), (0,)), ((), ())), preferred_element_type=jnp.float32).astype(jnp.bfloat16)
        dec[h : h + 1, :] = jnp.broadcast_to(end, (1, HEAD))
        if h == 0:
            steps(n - 1, 4, 5)
    for d in range(1, n):

        @pl.when(me + d < n)
        def _():
            state_copy(d).start()
            decay_copy(d).start()

    values = [acc[VALUE, :, h * HEAD : (h + 1) * HEAD].astype(jnp.bfloat16) for h in range(heads)]
    steps(n - 1, 5, 6)
    for h in range(heads):
        c = cum_s[:, h : h + 1]
        spread = c - cumt_s[h : h + 1, :]
        grid = jnp.where(below, jnp.exp(jnp.where(below, spread, 0.0)), 0.0)
        scores = lax.dot_general(qr[h], kr[h], (((1,), (1,)), ((), ())), preferred_element_type=jnp.float32) * grid
        kept_s[h] = jnp.dot(scores.astype(jnp.bfloat16), values[h], preferred_element_type=jnp.float32)
        if h == 0:
            steps(n - 1, 6, NPROJ)
    relay(n - 1)
    finish(3, 4)

    sin_s[...] = jnp.zeros_like(sin_s)
    for s in range(n - 1):

        @pl.when(me > s)
        def _():
            remote(lend, instate.at[s], ssend.at[0], srecv.at[s], "sp", s).wait_recv()
            remote(dec, indec.at[s], dsend.at[0], drecv.at[s], "sp", s).wait_recv()
            for h in range(heads):
                sin_s[h] = jnp.exp(indec[s, h : h + 1, :]) * sin_s[h] + instate[s, h].astype(jnp.float32)

    for h in range(heads):
        c = cum_s[:, h : h + 1]
        kept = kept_s[h]
        kept += jnp.dot(qr[h], sin_s[h].astype(jnp.bfloat16), preferred_element_type=jnp.float32) * jnp.exp(c)
        gate = projected(GATE, h)
        normed = kept * lax.rsqrt(jnp.mean(kept * kept, axis=-1, keepdims=True) + EPSILON)
        rb[:, h * HEAD : (h + 1) * HEAD] = (normed * (gate / (1.0 + jnp.exp(-gate)))).astype(jnp.bfloat16)

    def block(ref, to):
        return ref.at[pl.ds(pl.multiple_of(to * rows, rows), rows)]

    def branch_copy(kind, k):
        to = (twin, far, far_twin)[k]
        return remote(block((cb, rb)[kind], to), swap.at[kind, k], osend.at[kind, k], orecv.at[kind, k], "tp", to)

    for k in (1, 2, 0):
        branch_copy(1, k).start()

    finish(INNER, INPUT + 1)
    mixed_in = projected(INNER) * projected(INPUT)
    ext[8:, :] = mixed_in
    tail[...] = mixed_in[total - 8 :, :]

    def rim_copy():
        return remote(tail, ext.at[0:8], csend, crecv, "sp", me + 1)

    @pl.when(me < n - 1)
    def _():
        rim_copy().start()

    for d in range(1, n):
        at_distance(d, lambda s: [twin_copy(w, s).wait_recv() for w in range(2)])
        at_distance(d, lambda s: [relay_copy(w, s).wait_recv() for w in range(2)])
    for w in range(2):
        twin_copy(w, me).wait_recv()
        relay_copy(w, me).wait_recv()

    owners = (twin, far, far_twin)

    def add_branch(kind):
        at = pl.ds(pl.multiple_of(mine * rows, rows), rows)
        for k in range(m - 1):
            branch_copy(kind, k).wait_recv()
        parts = [(cb, rb)[kind][at, :]] + [swap[kind, k] for k in range(m - 1)]
        for s in range(n):
            to = slice(s * ocols, (s + 1) * ocols)
            value = jnp.dot(parts[0], go[mine, kind, s], preferred_element_type=jnp.float32)
            for k in range(m - 1):
                value += jnp.dot(parts[k + 1], go[owners[k], kind, s], preferred_element_type=jnp.float32)
            if kind == 1:
                own[:, to] = value
            else:
                out[:, to] = (own[:, to] + value).astype(jnp.bfloat16)

    add_branch(1)

    @pl.when(me > 0)
    def _():
        remote(tail, ext.at[0:8], csend, crecv, "sp", me - 1).wait_recv()

    @pl.when(me == 0)
    def _():
        ext[0:8, :] = jnp.zeros((8, cols), jnp.float32)

    t = taps[...].astype(jnp.float32)
    conv = jnp.zeros((total, cols), jnp.float32)
    for j in range(CONV_K):
        lo = 8 - (CONV_K - 1) + j
        conv = conv + t[j : j + 1, :] * ext[lo : lo + total, :]
    conv_s[...] = conv
    finish(OUTER, OUTER + 1)
    cb[...] = (projected(OUTER) * conv_s[...]).astype(jnp.bfloat16)
    for k in (1, 2, 0):
        branch_copy(0, k).start()
    add_branch(0)

    for k in range(m - 1):
        token_copy(k).wait_send()
        for kind in range(2):
            branch_copy(kind, k).wait_send()
    for w in range(2):
        for s in range(n):
            far_copy(w, s).wait_send()
            twin_copy(w, s).wait_send()
            relay_copy(w, s).wait_send()
    for d in range(1, n):

        @pl.when(me + d < n)
        def _():
            state_copy(d).wait_send()
            decay_copy(d).wait_send()

    @pl.when(me < n - 1)
    def _():
        rim_copy().wait_send()

    for is_out, count in ((True, 2), (False, NPROJ)):

        def drain(w, carry):
            for s in range(n):

                @pl.when((s <= me) & (me < n - 1))
                def _():
                    line_copy(w, s, is_out, True).wait_send()

                @pl.when((s >= me) & (me > 0))
                def _():
                    line_copy(w, s, is_out, False).wait_send()

                @pl.when(me != s)
                def _():
                    pair_copy(w, s, is_out).wait_send()

            return carry

        lax.fori_loop(0, count, drain, 0)


def fused(sizes, *args):
    n, g, m = sizes
    tokens, gain, w0 = args[0], args[1], args[2]
    log_decay = args[12]
    rows, width = tokens.shape
    depth, cols = w0.shape
    orows, ocols = args[10].shape
    total = rows * m
    heads = cols // HEAD
    bf, f32 = jnp.bfloat16, jnp.float32
    dma = pltpu.SemaphoreType.DMA
    scratch = [
        pltpu.VMEM((m - 1, rows, width), bf),
        pltpu.VMEM((n, total, depth), bf),
        pltpu.VMEM((NPROJ, n, depth, cols), bf),
        pltpu.VMEM((m, 2, n, orows, ocols), bf),
        pltpu.VMEM((NPROJ, total, cols), f32),
        pltpu.VMEM((total + 8, cols), f32),
        pltpu.VMEM((heads, total, HEAD), bf),
        pltpu.VMEM((heads, total, HEAD), bf),
        pltpu.VMEM((total, heads), f32),
        pltpu.VMEM((heads, total), f32),
        pltpu.VMEM((total, HEAD), f32),
        pltpu.VMEM((total, HEAD), f32),
        pltpu.VMEM((heads, total, HEAD), f32),
        pltpu.VMEM((total, cols), f32),
        pltpu.VMEM((heads, HEAD, HEAD), bf),
        pltpu.VMEM((8, HEAD), f32),
        pltpu.VMEM((n, heads, HEAD, HEAD), bf),
        pltpu.VMEM((n, 8, HEAD), f32),
        pltpu.VMEM((heads, HEAD, HEAD), f32),
        pltpu.VMEM((total, cols), bf),
        pltpu.VMEM((total, cols), bf),
        pltpu.VMEM((8, cols), f32),
        pltpu.VMEM((rows, width), f32),
        pltpu.VMEM((2, m - 1, rows, cols), bf),
        dma((m - 1,)),
        dma((m - 1,)),
        dma((NPROJ + 2, n)),
        dma((NPROJ + 2, n)),
        dma((NPROJ + 2, n)),
        dma((NPROJ + 2, n)),
        dma((NPROJ + 2, n)),
        dma((n,)),
        dma((n,)),
        dma((n,)),
        dma((n,)),
        dma,
        dma,
        dma((2, m - 1)),
        dma((2, m - 1)),
    ] + [dma((2, n))] * 6
    return pl.pallas_call(
        functools.partial(kernel, sizes),
        out_shape=jax.ShapeDtypeStruct((rows, width), bf),
        in_specs=[pl.BlockSpec(memory_space=pltpu.VMEM)] * 13,
        out_specs=pl.BlockSpec(memory_space=pltpu.VMEM),
        scratch_shapes=scratch,
        compiler_params=pltpu.CompilerParams(
            collective_id=0, has_side_effects=True, vmem_limit_bytes=60 * 1024 * 1024
        ),
    )(tokens, gain, *args[2:12], log_decay.T)


def solution(mesh):
    placed = (
        P(("grp", "sp", "tp"), None),
        P(),
        P("sp", "tp"),
        P("sp", "tp"),
        P("sp", "tp"),
        P("sp", "tp"),
        P("sp", "tp"),
        P("sp", "tp"),
        P("sp", "tp"),
        P(None, "tp"),
        P("tp", "sp"),
        P("tp", "sp"),
        P(("grp", "sp"), "tp"),
    )
    n, g, m = (mesh.shape[axis] for axis in ("sp", "grp", "tp"))
    fits = g == 2 and m == 4 and n == 4
    return jax.shard_map(
        functools.partial(fused, (n, g, m)) if fits else body, mesh=mesh, in_specs=placed, out_specs=P(("grp", "sp", "tp"), None), check_vma=False
    )
```
